512 devices in a mesh: grp: 2 (over y), sp: 32 (over z), tp: 8 (over x, core).
Axes of the slice: x: 4, y: 2, z: 32, core: 2. Of those that a mesh axis runs over, the one named last changes fastest.
The devices are a block of a 4x8x32 slice.
Arguments:
- tokens_in: bfloat16 [16384, 2048], P(('grp', 'sp')), parts along dimension 0, may hold values from -6 to 6
- input_gain: float32 [2048], replicated, may hold values from 0.1 to 1.9
- w_query: bfloat16 [2048, 1024], P('sp', 'tp'), may hold values from -0.125 to 0.125
- w_key: bfloat16 [2048, 1024], P('sp', 'tp'), may hold values from -1 to 1
- w_value: bfloat16 [2048, 1024], P('sp', 'tp'), may hold values from -0.125 to 0.125
- w_gates: bfloat16 [2048, 32], P('sp', 'tp'), may hold values from -3 to 3
- w_glu_value: bfloat16 [2048, 1024], P('sp', 'tp'), may hold values from -0.125 to 0.125
- sigmoid_opener_matrix: bfloat16 [2048, 1024], P('sp', 'tp'), may hold values from -0.125 to 0.125
- log_decay: float32 [16384, 16], P(('grp', 'sp'), 'tp'), parts along dimension 0, may hold values from -1 to 0
- head_gain: float32 [128], replicated, may hold values from 0.1 to 1.9
- conv_kernel: float32 [31, 1024], P(None, 'tp'), may hold values from -12 to 12
- norm_gain: float32 [1024], P('tp'), may hold values from 0.1 to 1.9
- norm_shift: float32 [1024], P('tp'), may hold values from -3 to 3
- out_delta: bfloat16 [2048, 1024], P(None, 'tp'), may hold values from -0.125 to 0.125
- out_conv: bfloat16 [2048, 1024], P(None, 'tp'), may hold values from -0.125 to 0.125
Outputs:
- mixed: bfloat16 [16384, 2048], P(('grp', 'sp'), 'tp'), parts along dimension 0
The draws below stay inside these ranges and needn't reach their ends.
There are 2 independent parts, one for each index of `grp`. The reference program is written for one: setup_inputs(seed, part) draws one part's arguments, and reference() takes and returns one part's arrays. A program takes and returns all parts, laid end to end along the dimension named above; an argument that names none is the same for every part. Nothing has to cross between parts.
All inputs are finite; a program needn't handle non-finite values.
Results may differ from the reference program's by a relative error of at most 0.015.
Values may be sent and summed in bfloat16 or wider, within the bound.
A program may use at most 64 MiB of HBM per device.

```python
import jax
import jax.numpy as jnp
from jax import lax

D = 2048
HEADS = 8
HEAD_DIM = 128
CONV_CH = 1024
KERNEL = 31
BLOCK = 64
TOK_DEV = 256
SEQ = 8192
A_W = 1024
N_TP = 8


def draw_log_decay(key, part):
    streams = jax.random.split(jax.random.fold_in(key, 11), 6)
    columns = 2 * HEADS
    fast_share = 0.5
    picker = jax.random.uniform(streams[0], (columns,), jnp.float32)
    fast_rate = jax.random.uniform(streams[1], (columns,), jnp.float32, 0.015, 0.04)
    slow_rate = jax.random.uniform(streams[2], (columns,), jnp.float32, 0.04, 0.16) / SEQ
    forgetting_pace = jnp.where(picker < fast_share, fast_rate, slow_rate)
    multiplier_amount = jnp.exp(jax.random.uniform(streams[3], (SEQ // TOK_DEV, columns), jnp.float32, 0.0, 1.0986))
    multiplier_amount = jnp.repeat(multiplier_amount, TOK_DEV, axis=0)
    spots = jax.random.randint(streams[4], (2, columns), 0, SEQ)
    places = jnp.arange(SEQ)[:, None]
    masked_elements = (places == spots[0][None, :]) | (places == spots[1][None, :])
    objective_readings = jax.random.uniform(streams[5], (SEQ, columns), jnp.float32, 0.2, 0.35)
    clustered_bunches = jnp.where(masked_elements, jnp.log(1.0 - objective_readings), 0.0)
    return (-(forgetting_pace[None, :] * multiplier_amount) + clustered_bunches).astype(jnp.float32)


def draw_conv_kernel(key, part):
    streams = jax.random.split(jax.random.fold_in(key, 23), 2)
    channel_slot = jnp.arange(CONV_CH).astype(jnp.float32)
    random_perturbation = jax.random.uniform(streams[1], (CONV_CH,), jnp.float32)
    entries = jnp.clip(jax.random.normal(streams[0], (KERNEL, CONV_CH), jnp.float32), -4.0, 4.0)
    reach = 10.0
    scale = reach ** ((channel_slot + random_perturbation) / CONV_CH)
    return (entries * scale[None, :] / jnp.sqrt(float(KERNEL))).astype(jnp.float32)


def unit_entries(stream, shape):
    return jnp.clip(jax.random.normal(stream, shape, jnp.float32), -4.0, 4.0)


def draw_w_key(key, part):
    streams = jax.random.split(jax.random.fold_in(key, 31), 2)
    strong_count = HEAD_DIM * 3 // 8
    weak_energy = 0.356 * (HEAD_DIM - strong_count)
    ratio_square = max(1.0, (0.04 * SEQ - weak_energy) / (0.5 * strong_count))
    orders = jax.vmap(lambda sub_key: jax.random.permutation(sub_key, HEAD_DIM))(jax.random.split(streams[0], HEADS))
    column_scale = jnp.where(orders < strong_count, ratio_square ** 0.5, 1.0).reshape(HEADS * HEAD_DIM).astype(jnp.float32)
    entries = unit_entries(streams[1], (D, HEADS * HEAD_DIM))
    return (entries * column_scale[None, :] / jnp.sqrt(float(D))).astype(jnp.bfloat16)


def draw_w_gates(key, part):
    stream = jax.random.fold_in(key, 37)
    roles = jnp.arange(4 * HEADS) % 4
    column_scale = jnp.where((roles == 1) | (roles == 3), 4.0, 1.0).astype(jnp.float32)
    entries = unit_entries(stream, (D, 4 * HEADS))
    return (entries * column_scale[None, :] / jnp.sqrt(float(D))).astype(jnp.bfloat16)


def shard_levels(key, extent, shards, smallest, top_value):
    level = 1.0
    for axis_at, parts in shards:
        heights = jax.random.uniform(jax.random.fold_in(jax.random.fold_in(key, 6), axis_at), (parts,), jnp.float32, smallest / len(shards), top_value / len(shards))
        level = level * jnp.repeat(jnp.exp(heights), extent[axis_at] // parts).reshape((-1,) + (1,) * (len(extent) - 1 - axis_at))
    return level


def bell_draw(rng, dims, scale, most, cuts=(), kind=jnp.bfloat16):
    array = jax.random.normal(rng, dims, jnp.float32) * scale
    if len(cuts) > 0:
        array = shard_levels(rng, dims, cuts, -0.22, 0.18) * array
    return jnp.clip(array, min=-most, max=most).astype(kind)


def setup_inputs(seed: int = 0, part: int = 0) -> dict:
    key_list = jax.random.split(jax.random.key(seed), 16)
    part_keys = jax.random.split(jax.random.fold_in(key_list[15], part), 16)
    tokens_in = bell_draw(part_keys[0], (SEQ, D), 1.0, 6.0, ((0, 32),))
    input_gain = jnp.clip(1.0 + 0.18 * jax.random.normal(key_list[1], (D,), jnp.float32), 0.1, 1.9)
    w_query = bell_draw(key_list[2], (D, A_W), D ** -0.5, 0.125, ((0, 32), (1, 8)))
    w_key = draw_w_key(jax.random.fold_in(key_list[15], 71), part)
    w_value = bell_draw(key_list[4], (D, A_W), D ** -0.5, 0.125, ((0, 32), (1, 8)))
    w_gates = draw_w_gates(jax.random.fold_in(key_list[15], 71), part)
    w_glu_value = bell_draw(key_list[6], (D, CONV_CH), D ** -0.5, 0.125, ((0, 32), (1, 8)))
    sigmoid_opener_matrix = bell_draw(key_list[7], (D, CONV_CH), D ** -0.5, 0.125, ((0, 32), (1, 8)))
    log_decay = draw_log_decay(jax.random.fold_in(jax.random.fold_in(key_list[15], part), 71), part)
    head_gain = jnp.clip(1.0 + 0.18 * jax.random.normal(key_list[9], (HEAD_DIM,), jnp.float32), 0.1, 1.9)
    conv_kernel = draw_conv_kernel(jax.random.fold_in(key_list[15], 71), part)
    norm_gain = jnp.clip(1.0 + 0.18 * jax.random.normal(key_list[11], (CONV_CH,), jnp.float32), 0.1, 1.9)
    norm_shift = bell_draw(key_list[12], (CONV_CH,), 0.5, 3.0, ((0, 8),), jnp.float32)
    out_delta = bell_draw(key_list[13], (D, A_W), (A_W + CONV_CH) ** -0.5, 0.125, ((1, 8),))
    out_conv = bell_draw(key_list[14], (D, CONV_CH), (A_W + CONV_CH) ** -0.5, 0.125, ((1, 8),))
    return {"tokens_in": tokens_in, "input_gain": input_gain, "w_query": w_query, "w_key": w_key, "w_value": w_value, "w_gates": w_gates, "w_glu_value": w_glu_value, "sigmoid_opener_matrix": sigmoid_opener_matrix, "log_decay": log_decay, "head_gain": head_gain, "conv_kernel": conv_kernel, "norm_gain": norm_gain, "norm_shift": norm_shift, "out_delta": out_delta, "out_conv": out_conv}


PRECISE = lax.Precision.HIGHEST
EPSILON = 1e-06
BETA_SHIFT = 6.0

def high_dot(left, right):
    return jnp.matmul(left, right, precision=PRECISE)

def swap_last(tensor):
    return jnp.swapaxes(tensor, -1, -2)

def block_terms(query, key_rows, values, decay_log, beta_rate, block):
    head_count, length = (query.shape[0], query.shape[1])
    blocks = length // block

    def to_blocks(tensor):
        return tensor.reshape((head_count, blocks, block) + tensor.shape[2:])
    query, key_rows, values, decay_log, beta_rate = (to_blocks(tensor) for tensor in (query, key_rows, values, decay_log, beta_rate))
    cumulative = jnp.cumsum(decay_log, axis=-1)
    positions = jnp.arange(block)
    on_or_below = positions[:, None] >= positions[None, :]
    strict = positions[:, None] > positions[None, :]
    log_gaps = cumulative[..., :, None] - cumulative[..., None, :]
    weighting = jnp.where(on_or_below, jnp.exp(jnp.where(on_or_below, log_gaps, 0.0)), 0.0)
    scaled_keys = key_rows * beta_rate[..., None]
    lower_part = jnp.where(strict, high_dot(scaled_keys, swap_last(key_rows)) * weighting, 0.0)
    identity = jnp.eye(block, dtype=jnp.float32)
    inverse = jax.scipy.linalg.solve_triangular(identity + lower_part, jnp.broadcast_to(identity, lower_part.shape), lower=True, unit_diagonal=True)
    update = high_dot(inverse, values * beta_rate[..., None])
    mixed_keys = high_dot(inverse, scaled_keys * jnp.exp(cumulative)[..., None])
    in_block = jnp.where(on_or_below, high_dot(query, swap_last(key_rows)) * weighting, 0.0)
    q_decayed = query * jnp.exp(cumulative)[..., None]
    k_decayed = key_rows * jnp.exp(cumulative[..., -1:] - cumulative)[..., None]
    end_decay = jnp.exp(cumulative[..., -1])
    return tuple((jnp.moveaxis(tensor, 1, 0) for tensor in (update, mixed_keys, in_block, q_decayed, k_decayed, end_decay)))

def delta_scan(query, key_rows, values, decay_log, beta_rate):
    stacked = block_terms(query, key_rows, values, decay_log, beta_rate, BLOCK)
    head_count, length, head_width = query.shape

    def advance(state_now, pieces):
        update, mixed_keys, in_block, q_decayed, k_decayed, end_decay = pieces
        new_values = update - high_dot(mixed_keys, state_now)
        output = high_dot(q_decayed, state_now) + high_dot(in_block, new_values)
        state_now = state_now * end_decay[:, None, None] + high_dot(swap_last(k_decayed), new_values)
        return (state_now, output)
    zero_state = jnp.zeros((head_count, head_width, values.shape[2]), jnp.float32)
    _, output = lax.scan(advance, zero_state, stacked)
    return jnp.moveaxis(output, 0, 1).reshape(head_count, length, values.shape[2])

def reference(tokens_in, input_gain, w_query, w_key, w_value, w_gates, w_glu_value, sigmoid_opener_matrix, log_decay, head_gain, conv_kernel, norm_gain, norm_shift, out_delta, out_conv):
    rows = tokens_in.astype(jnp.float32)
    normed = (rows * lax.rsqrt(lax.optimization_barrier(jnp.mean(rows * rows, axis=-1, keepdims=True)) + EPSILON) * input_gain).astype(jnp.bfloat16)

    def project(weight):
        return jnp.dot(normed.astype(jnp.float32), weight.astype(jnp.float32), preferred_element_type=jnp.float32)

    def by_head(tensor):
        return jnp.swapaxes(jax.nn.silu(tensor).reshape(SEQ, HEADS, HEAD_DIM), 0, 1)

    def unit_rows(tensor):
        return tensor * lax.rsqrt(lax.optimization_barrier(jnp.sum(tensor * tensor, axis=-1, keepdims=True)) + EPSILON)
    query = unit_rows(by_head(project(w_query))) * HEAD_DIM ** (-0.5)
    key_rows = unit_rows(by_head(project(w_key)))
    values = by_head(project(w_value))
    gate_parts = project(w_gates).reshape(SEQ, HEADS, 4)
    rate_parts = log_decay.reshape(SEQ, HEADS, 2)
    decay_fore = jnp.swapaxes(rate_parts[:, :, 0] * (0.5 + jax.nn.sigmoid(gate_parts[:, :, 0])), 0, 1)
    beta_fore = jnp.swapaxes(jax.nn.sigmoid(gate_parts[:, :, 1] - BETA_SHIFT), 0, 1)
    decay_back = jnp.swapaxes(rate_parts[:, :, 1] * (0.5 + jax.nn.sigmoid(gate_parts[:, :, 2])), 0, 1)
    beta_back = jnp.swapaxes(jax.nn.sigmoid(gate_parts[:, :, 3] - BETA_SHIFT), 0, 1)

    def reversed_rows(tensor):
        return jnp.flip(tensor, axis=1)
    fore = delta_scan(query, key_rows, values, decay_fore, beta_fore)
    back = reversed_rows(delta_scan(reversed_rows(query), reversed_rows(key_rows), reversed_rows(values), reversed_rows(decay_back), reversed_rows(beta_back)))
    joined = fore + back
    joined = joined * lax.rsqrt(lax.optimization_barrier(jnp.mean(joined * joined, axis=-1, keepdims=True)) + EPSILON) * head_gain
    delta_mix = jnp.swapaxes(joined, 0, 1).reshape(SEQ, HEADS * HEAD_DIM).astype(jnp.bfloat16)
    glu_rows = (project(w_glu_value) * jax.nn.sigmoid(project(sigmoid_opener_matrix))).astype(jnp.bfloat16)
    half_width = KERNEL // 2
    padded = jnp.pad(glu_rows.astype(jnp.float32), ((half_width, half_width), (0, 0)))
    conv_rows = padded[0:SEQ] * conv_kernel[0]
    for offset in range(1, KERNEL):
        conv_rows = conv_rows + padded[offset:offset + SEQ] * conv_kernel[offset]
    center = lax.optimization_barrier(jnp.mean(conv_rows, axis=-1))
    spread = lax.optimization_barrier(jnp.mean(conv_rows * conv_rows, axis=-1)) - center * center
    normal_rows = (conv_rows - center[:, None]) * lax.rsqrt(spread + EPSILON)[:, None]
    filtered_blend = jax.nn.silu(normal_rows * norm_gain + norm_shift).astype(jnp.bfloat16)
    head_cols = HEADS * HEAD_DIM // N_TP
    channel_columns = CONV_CH // N_TP
    result = jnp.zeros((SEQ, D), jnp.float32)
    for group in range(N_TP):
        partial_sum = jnp.dot(delta_mix[:, group * head_cols:(group + 1) * head_cols].astype(jnp.float32), out_delta[:, group * head_cols:(group + 1) * head_cols].T.astype(jnp.float32), preferred_element_type=jnp.float32)
        partial_sum = partial_sum + jnp.dot(filtered_blend[:, group * channel_columns:(group + 1) * channel_columns].astype(jnp.float32), out_conv[:, group * channel_columns:(group + 1) * channel_columns].T.astype(jnp.float32), preferred_element_type=jnp.float32)
        rounded = lax.optimization_barrier(partial_sum.astype(jnp.bfloat16))
        result = result + rounded.astype(jnp.float32)
    return result.astype(jnp.bfloat16)
```

```python
import functools

import jax
import jax.numpy as jnp
from jax import lax
from jax.experimental import pallas as pl
from jax.experimental.pallas import tpu as pltpu
from jax.sharding import PartitionSpec as P

EPSILON = 1e-06
BETA_SHIFT = 6.0
SPAN = 4
PARTS = 2
MESH = pl.DeviceIdType.MESH
F32 = jnp.float32
BF16 = jnp.bfloat16


def dot(a, b, dims=((1,), (0,))):
    return lax.dot_general(a, b, (dims, ((), ())), preferred_element_type=F32)


def bf_dot(a, b, dims=((1,), (0,))):
    return dot(a.astype(BF16), b.astype(BF16), dims)


def split(a):
    high = a.astype(BF16)
    return high, (a - high.astype(F32)).astype(BF16)


def fine_dot(a, b, dims=((1,), (0,))):
    ah, al = split(a)
    bh, bl = split(b)
    return dot(ah, bh, dims) + (dot(al, bh, dims) + dot(ah, bl, dims))


def mask_dot(mask, b):
    high, rest = split(b)
    middle = b - high.astype(F32) - rest.astype(F32)
    return dot(mask, high) + (dot(mask, rest) + dot(mask, middle.astype(BF16)))


def sigmoid(a):
    return 1.0 / (1.0 + jnp.exp(-a))


def silu(a):
    return a * sigmoid(a)


def unit_rows(a):
    return a * lax.rsqrt(jnp.sum(a * a, axis=-1, keepdims=True) + EPSILON)


def unit_inverse(a):
    size = a.shape[0]
    row = lax.broadcasted_iota(jnp.int32, (size, size), 0)
    col = lax.broadcasted_iota(jnp.int32, (size, size), 1)
    apart = row ^ col
    inverse = jnp.where(row == col, 1.0, jnp.where(apart < 2, -a, 0.0))
    half = 2
    while half < size:
        corner = jnp.where((apart >= half) & (apart < 2 * half), a, 0.0)
        inverse = inverse - fine_dot(inverse, fine_dot(corner, inverse))
        half *= 2
    return inverse


def triangular_inverse(a, upper):
    half = a.shape[0] // 2
    first = unit_inverse(a[:half, :half])
    second = unit_inverse(a[half:, half:])
    zero = jnp.zeros((half, half), F32)
    if upper:
        corner = -fine_dot(first, fine_dot(a[:half, half:], second))
        rows = (jnp.concatenate([first, corner], 1), jnp.concatenate([zero, second], 1))
    else:
        corner = -fine_dot(second, fine_dot(a[half:, :half], first))
        rows = (jnp.concatenate([first, zero], 1), jnp.concatenate([corner, second], 1))
    return jnp.concatenate(rows, 0)


def delta_block(query, key_rows, values, keys_keys, query_keys, total_col, total_row, beta, upper):
    length, width = key_rows.shape
    row = lax.broadcasted_iota(jnp.int32, (length, length), 0)
    col = lax.broadcasted_iota(jnp.int32, (length, length), 1)
    within = (col >= row) if upper else (row >= col)
    weighting = jnp.where(within, jnp.exp(jnp.minimum(total_col - total_row, 0.0)), 0.0)
    coupling = jnp.where(row == col, 0.0, beta * keys_keys * weighting)
    inverse = triangular_inverse(coupling, upper)
    decayed = jnp.exp(total_col)
    sources = jnp.concatenate([beta * values, (beta * decayed) * key_rows], 1)
    sources = bf_dot(inverse, sources).astype(BF16)
    here = bf_dot(query_keys * weighting, sources)
    end = total_col[0:1, :] if upper else total_col[length - 1 :, :]
    leaving = key_rows * jnp.exp(end - total_col)
    update = bf_dot(leaving, sources, ((0,), (0,)))
    eye = jnp.where(
        lax.broadcasted_iota(jnp.int32, (width, width), 0)
        == lax.broadcasted_iota(jnp.int32, (width, width), 1),
        1.0,
        0.0,
    )
    state_map = jnp.exp(end) * eye - update[:, width:]
    reading = query * decayed - here[:, width:]
    return here[:, :width], reading, jnp.concatenate([state_map, update[:, :width]], 1)


def layer_kernel(
    nz,
    nt,
    x_ref,
    gain_ref,
    wq_ref,
    wk_ref,
    wv_ref,
    wg_ref,
    wc_ref,
    ws_ref,
    decay_ref,
    head_gain_ref,
    taps_ref,
    norm_gain_ref,
    norm_shift_ref,
    od_ref,
    oc_ref,
    out_ref,
    w_buf,
    g_buf,
    od_buf,
    oc_buf,
    fd_buf,
    fc_buf,
    stat_buf,
    normed_ref,
    proj_ref,
    glu_ref,
    halo_ref,
    pad_ref,
    square_ref,
    local_ref,
    read_ref,
    own_ref,
    near_ref,
    prefix_ref,
    head_ref,
    far_ref,
    state_ref,
    enter_send,
    enter_ref,
    load_sem,
    ring_send,
    ring_recv,
    gate_send,
    gate_recv,
    out_send,
    out_recv,
    halo_send,
    halo_recv,
    stat_send,
    stat_recv,
    fc_send,
    fc_recv,
    fd_send,
    fd_recv,
    near_send,
    near_recv,
    far_send,
    far_recv,
    enter_send_sem,
    enter_recv,
):
    z = lax.axis_index("sp")
    t = lax.axis_index("tp")
    rows = wq_ref.shape[0]
    length = x_ref.shape[0]
    width = wq_ref.shape[1]
    out_cols = out_ref.shape[1]
    piece = rows // PARTS
    blocks = nz // SPAN
    right = lax.rem(z + 1, nz)
    left = lax.rem(z + nz - 1, nz)
    ups = nz // 2
    downs = nz - 1 - ups

    def to(zz, tt):
        return {"sp": zz, "tp": tt}

    def remote(src, dst, send, recv, where):
        return pltpu.make_async_remote_copy(
            src_ref=src,
            dst_ref=dst,
            send_sem=send,
            recv_sem=recv,
            device_id=where,
            device_id_type=MESH,
        )

    def lane_block(index):
        return pl.ds(pl.multiple_of(index * width, width), width)

    loads = []
    base = pl.multiple_of(z * rows, rows)
    for n, src in enumerate((wk_ref, wv_ref, wq_ref, wc_ref, ws_ref)):
        loads.append(
            pltpu.make_async_copy(
                src,
                w_buf.at[pl.ds(base, rows), pl.ds(n * width, width)],
                load_sem.at[n],
            )
        )
    loads.append(pltpu.make_async_copy(od_ref.at[pl.ds(pl.multiple_of(t * out_cols, out_cols), out_cols), :], od_buf.at[:, lane_block(t)], load_sem.at[5]))
    loads.append(pltpu.make_async_copy(oc_ref.at[pl.ds(pl.multiple_of(t * out_cols, out_cols), out_cols), :], oc_buf.at[:, lane_block(t)], load_sem.at[6]))
    for load in loads:
        load.start()

    square_ref[...] = jnp.zeros_like(square_ref)
    square_ref[0:rows, 0:4] = wg_ref[...].astype(F32)
    flat = jnp.transpose(square_ref[0:width, :])[0:16, :]
    if 2 * rows == width:
        odd = lax.rem(z, 2) == 1
        flat = jnp.where(odd, pltpu.roll(flat, rows, 1), flat)
    g_buf[z] = flat.astype(BF16)

    barrier = pltpu.get_barrier_semaphore()
    pl.semaphore_signal(barrier, inc=1, device_id=to(right, t), device_id_type=MESH)
    pl.semaphore_signal(barrier, inc=1, device_id=to(left, t), device_id_type=MESH)
    for d in range(1, nt):
        pl.semaphore_signal(
            barrier, inc=1, device_id=to(z, lax.rem(t + d, nt)), device_id_type=MESH
        )
    pl.semaphore_wait(barrier, nt + 1)
    for load in loads:
        load.wait()

    def chunk_copy(origin, part, way, step):
        at = pl.ds(pl.multiple_of(origin * rows + part * piece, piece), piece)
        return remote(
            w_buf.at[at, :],
            w_buf.at[at, :],
            ring_send.at[way, step, part],
            ring_recv.at[way, step, part],
            to((right, left)[way], t),
        )

    def gate_copy(origin, way, step):
        return remote(
            g_buf.at[origin],
            g_buf.at[origin],
            gate_send.at[way, step],
            gate_recv.at[way, step],
            to((right, left)[way], t),
        )

    for part in range(PARTS):
        chunk_copy(z, part, 0, 0).start()
        chunk_copy(z, part, 1, 0).start()
    gate_copy(z, 0, 0).start()
    gate_copy(z, 1, 0).start()

    def out_copy(d):
        owner = lax.rem(t + d, nt)
        block = pl.ds(pl.multiple_of(owner * out_cols, out_cols), out_cols)
        return (
            remote(od_ref.at[block, :], od_buf.at[:, lane_block(t)], out_send.at[0, d - 1], out_recv.at[0, d - 1], to(z, owner)),
            remote(oc_ref.at[block, :], oc_buf.at[:, lane_block(t)], out_send.at[1, d - 1], out_recv.at[1, d - 1], to(z, owner)),
        )

    for d in range(1, nt):
        for copy in out_copy(d):
            copy.start()

    x = x_ref[...].astype(F32)
    scale = lax.rsqrt(jnp.mean(x * x, axis=-1, keepdims=True) + EPSILON)
    normed_ref[...] = (x * scale * gain_ref[...]).astype(BF16)

    def ring_step(step, carry):
        up = lax.rem(z + nz - step, nz)
        down = lax.rem(z + step, nz)
        for part in range(PARTS):
            chunk_copy(up, part, 0, step - 1).wait_recv()
            chunk_copy(up, part, 0, step).start()
            chunk_copy(down, part, 1, step - 1).wait_recv()

            @pl.when(step < downs)
            def _():
                chunk_copy(down, part, 1, step).start()

        gate_copy(up, 0, step - 1).wait_recv()
        gate_copy(up, 0, step).start()
        gate_copy(down, 1, step - 1).wait_recv()

        @pl.when(step < downs)
        def _():
            gate_copy(down, 1, step).start()

        return carry

    lax.fori_loop(1, ups, ring_step, 0)
    last = lax.rem(z + nz - ups, nz)
    for part in range(PARTS):
        chunk_copy(last, part, 0, ups - 1).wait_recv()
    gate_copy(last, 0, ups - 1).wait_recv()

    normed = normed_ref[...]
    proj_ref[...] = dot(normed, w_buf[...])
    gate_rows = jnp.concatenate(
        [
            g_buf[2 * m] + g_buf[2 * m + 1] if 2 * rows == width else g_buf[m]
            for m in range(nz * rows // width)
        ],
        1,
    )
    gates = dot(normed, gate_rows, ((1,), (1,)))

    glu = (proj_ref[:, 3 * width : 4 * width] * sigmoid(proj_ref[:, 4 * width :])).astype(BF16)
    glu_ref[...] = glu
    edge = halo_ref.shape[1]
    edge_up = remote(glu_ref.at[pl.ds(length - edge, edge), :], halo_ref.at[0], halo_send.at[0], halo_recv.at[0], to(right, t))
    edge_down = remote(glu_ref.at[pl.ds(0, edge), :], halo_ref.at[1], halo_send.at[1], halo_recv.at[1], to(left, t))
    edge_up.start()
    edge_down.start()

    key_rows = unit_rows(silu(proj_ref[:, 0:width]))
    values = silu(proj_ref[:, width : 2 * width])
    query = unit_rows(silu(proj_ref[:, 2 * width : 3 * width])) * width ** (-0.5)
    lane = lax.broadcasted_iota(jnp.int32, gates.shape, 1)
    shift = jnp.where((lane == 1) | (lane == 3), BETA_SHIFT, 0.0)
    opened = sigmoid(gates - shift)
    base_decay = jnp.where(
        lane == 0, decay_ref[:, 0:1], jnp.where(lane == 2, decay_ref[:, 1:2], 0.0)
    )
    decays = base_decay * (0.5 + opened)
    row = lax.broadcasted_iota(jnp.int32, (length, length), 0)
    col = lax.broadcasted_iota(jnp.int32, (length, length), 1)
    below = jnp.where(row >= col, 1.0, 0.0).astype(BF16)
    above = jnp.where(col >= row, 1.0, 0.0).astype(BF16)
    totals = jnp.where(lane == 0, mask_dot(below, decays), mask_dot(above, decays))
    square_ref[:, 0 : gates.shape[1]] = totals
    total_rows = jnp.transpose(square_ref[...])
    keys_keys = fine_dot(key_rows, key_rows, ((1,), (1,)))
    query_keys = bf_dot(query, key_rows, ((1,), (1,)))
    here = []
    for way in (0, 1):
        output, reading, affine = delta_block(
            query,
            key_rows,
            values,
            keys_keys,
            query_keys,
            totals[:, 2 * way : 2 * way + 1],
            total_rows[2 * way : 2 * way + 1, :],
            opened[:, 2 * way + 1 : 2 * way + 2],
            way == 1,
        )
        here.append(output)
        read_ref[way] = reading.astype(BF16)
        own_ref[way] = affine.astype(BF16)
    local_ref[...] = here[0] + here[1]

    place = lax.rem(z, SPAN)
    block = z // SPAN
    near = []
    for d in range(SPAN - 1, 0, -1):
        for way in (0, 1):
            fits = (place + d < SPAN) if way == 0 else (place >= d)
            target = lax.rem(z + (d if way == 0 else nz - d), nz)
            copy = remote(own_ref.at[way], near_ref.at[way, place], near_send.at[way, d - 1], near_recv.at[way, d - 1], to(target, t))
            near.append((fits, copy))

            @pl.when(fits)
            def _():
                copy.start()

    edge_up.wait_recv()
    edge_down.wait_recv()
    taps = taps_ref.shape[0]
    half_width = taps // 2
    pad_ref[0:edge, :] = jnp.where(z == 0, 0.0, halo_ref[0].astype(F32))
    pad_ref[edge : edge + length, :] = glu_ref[...].astype(F32)
    pad_ref[edge + length :, :] = jnp.where(z == nz - 1, 0.0, halo_ref[1].astype(F32))
    start = edge - half_width
    conv = pad_ref[start : start + length, :] * taps_ref[0:1, :]
    for offset in range(1, taps):
        conv = conv + pad_ref[start + offset : start + offset + length, :] * taps_ref[offset : offset + 1, :]
    square_ref[:, 0:1] = jnp.sum(conv, axis=-1, keepdims=True)
    square_ref[:, 1:2] = jnp.sum(conv * conv, axis=-1, keepdims=True)
    stat_buf[t] = jnp.transpose(square_ref[...])[0:8, :]

    def stat_copy(d):
        return remote(stat_buf.at[t], stat_buf.at[t], stat_send.at[d - 1], stat_recv.at[d - 1], to(z, lax.rem(t + d, nt)))

    for d in range(1, nt):
        stat_copy(d).start()
    proj_ref[:, 0:width] = conv

    for way in (0, 1):
        eye = jnp.where(
            lax.broadcasted_iota(jnp.int32, (width, 2 * width), 0)
            == lax.broadcasted_iota(jnp.int32, (width, 2 * width), 1),
            1.0,
            0.0,
        )
        prefix_ref[way] = eye
    right_part = lax.broadcasted_iota(jnp.int32, (width, 2 * width), 1) >= width

    def compose(affine, before):
        return bf_dot(affine[:, 0:width], before) + jnp.where(right_part, affine.astype(F32), 0.0)

    for step in range(SPAN - 1):
        for way in (0, 1):
            origin = step if way == 0 else SPAN - 1 - step
            comes = (place > origin) if way == 0 else (place < origin)
            distance = (place - origin) if way == 0 else (origin - place)

            @pl.when(comes)
            def _():
                remote(
                    own_ref.at[way],
                    near_ref.at[way, origin],
                    near_send.at[way, 0],
                    near_recv.at[way, distance - 1],
                    to(right, t),
                ).wait_recv()
                prefix_ref[way] = compose(near_ref[way, origin], prefix_ref[way])

    def leads(way):
        if way == 0:
            return (place == SPAN - 1) & (block < blocks - 1)
        return (place == 0) & (block > 0)

    def far_copy(way, d):
        target = lax.rem(z + (SPAN * d if way == 0 else nz - SPAN * d), nz)
        return remote(head_ref.at[way], far_ref.at[way, block], far_send.at[way, d - 1], far_recv.at[way, d - 1], to(target, t))

    def far_fits(way, d):
        if way == 0:
            return leads(way) & (block + d < blocks - 1)
        return leads(way) & (block - d > 0)

    for way in (0, 1):

        @pl.when(leads(way))
        def _():
            head_ref[way] = compose(own_ref[way], prefix_ref[way]).astype(BF16)

    for d in range(blocks - 2, 0, -1):
        for way in (0, 1):

            @pl.when(far_fits(way, d))
            def _():
                far_copy(way, d).start()

    total = stat_buf[t]
    for d in range(1, nt):
        stat_copy(d).wait_recv()
    for d in range(1, nt):
        total = total + stat_buf[lax.rem(t + nt - d, nt)]
    square_ref[0:width, :] = jnp.zeros((width, width), F32)
    stats = jnp.transpose(jnp.concatenate([total, jnp.zeros((width - 8, length), F32)], 0))
    channels = nt * width
    center = stats[:, 0:1] / channels
    spread = stats[:, 1:2] / channels - center * center
    normal = (proj_ref[:, 0:width] - center) * lax.rsqrt(spread + EPSILON)
    fc_buf[:, lane_block(t)] = silu(normal * norm_gain_ref[...] + norm_shift_ref[...]).astype(BF16)

    def feature_copy(buf, send, recv, d):
        return remote(buf.at[:, lane_block(t)], buf.at[:, lane_block(t)], send.at[d - 1], recv.at[d - 1], to(z, lax.rem(t + d, nt)))

    for d in range(1, nt):
        feature_copy(fc_buf, fc_send, fc_recv, d).start()

    for way in (0, 1):

        @pl.when(leads(way))
        def _():
            state_ref[way] = jnp.zeros((width, width), F32)

    for step in range(blocks - 2):
        for way in (0, 1):
            origin = step if way == 0 else blocks - 1 - step
            comes = leads(way) & ((block > origin) if way == 0 else (block < origin))
            distance = (block - origin) if way == 0 else (origin - block)

            @pl.when(comes)
            def _():
                remote(
                    head_ref.at[way],
                    far_ref.at[way, origin],
                    far_send.at[way, 0],
                    far_recv.at[way, distance - 1],
                    to(right, t),
                ).wait_recv()
                affine = far_ref[way, origin]
                state_ref[way] = bf_dot(affine[:, 0:width], state_ref[way]) + affine[:, width:].astype(F32)

    def enter_copy(way, d):
        target = lax.rem(z + (d if way == 0 else nz - d), nz)
        slot = (d - 1) if way == 0 else (SPAN - d)
        return remote(enter_send.at[way], enter_ref.at[way], enter_send_sem.at[way, d - 1], enter_recv.at[way], to(target, t))

    for way in (0, 1):

        @pl.when(leads(way))
        def _():
            affine = head_ref[way]
            state = bf_dot(affine[:, 0:width], state_ref[way]) + affine[:, width:].astype(F32)
            enter_send[way] = state.astype(BF16)
            for d in range(SPAN, 0, -1):
                enter_copy(way, d).start()

    for d in range(1, nt):
        for copy in out_copy(d):
            copy.wait_recv()
        feature_copy(fc_buf, fc_send, fc_recv, d).wait_recv()
    mixed = dot(fc_buf[...], oc_buf[...], ((1,), (1,)))

    for way in (0, 1):
        state_ref[way] = prefix_ref[way][:, width:]
        follows = (block > 0) if way == 0 else (block < blocks - 1)

        @pl.when(follows)
        def _():
            enter_copy(way, 1).wait_recv()
            state_ref[way] = state_ref[way] + bf_dot(prefix_ref[way][:, 0:width], enter_ref[way])

    joined = local_ref[...]
    for way in (0, 1):
        joined = joined + bf_dot(read_ref[way], state_ref[way])
    joined = joined * lax.rsqrt(jnp.mean(joined * joined, axis=-1, keepdims=True) + EPSILON)
    fd_buf[:, lane_block(t)] = (joined * head_gain_ref[...]).astype(BF16)
    for d in range(1, nt):
        feature_copy(fd_buf, fd_send, fd_recv, d).start()
    for d in range(1, nt):
        feature_copy(fd_buf, fd_send, fd_recv, d).wait_recv()
    out_ref[...] = (mixed + dot(fd_buf[...], od_buf[...], ((1,), (1,)))).astype(BF16)

    def drain(step, carry):
        for part in range(PARTS):
            chunk_copy(z, part, 0, step).wait_send()
        gate_copy(z, 0, step).wait_send()

        @pl.when(step < downs)
        def _():
            for part in range(PARTS):
                chunk_copy(z, part, 1, step).wait_send()
            gate_copy(z, 1, step).wait_send()

        return carry

    lax.fori_loop(0, ups, drain, 0)
    edge_up.wait_send()
    edge_down.wait_send()
    for d in range(1, nt):
        for copy in out_copy(d):
            copy.wait_send()
        stat_copy(d).wait_send()
        feature_copy(fc_buf, fc_send, fc_recv, d).wait_send()
        feature_copy(fd_buf, fd_send, fd_recv, d).wait_send()
    for fits, copy in near:

        @pl.when(fits)
        def _():
            copy.wait_send()

    for way in (0, 1):
        for d in range(blocks - 2, 0, -1):

            @pl.when(far_fits(way, d))
            def _():
                far_copy(way, d).wait_send()

        @pl.when(leads(way))
        def _():
            for d in range(SPAN, 0, -1):
                enter_copy(way, d).wait_send()


def on_device(
    nz,
    nt,
    tokens_in,
    input_gain,
    w_query,
    w_key,
    w_value,
    w_gates,
    w_glu_value,
    sigmoid_opener_matrix,
    log_decay,
    head_gain,
    conv_kernel,
    norm_gain,
    norm_shift,
    out_delta,
    out_conv,
):
    length, features = tokens_in.shape
    rows, width = w_query.shape
    out_cols = out_delta.shape[0] // nt
    blocks = nz // SPAN
    ups = nz // 2
    edge = 16
    vmem = pl.BlockSpec(memory_space=pltpu.VMEM)
    hbm = pl.BlockSpec(memory_space=pl.ANY)
    dma = pltpu.SemaphoreType.DMA
    scratch = [
        pltpu.VMEM((nz * rows, 5 * width), BF16),
        pltpu.VMEM((nz, 16, width), BF16),
        pltpu.VMEM((out_cols, nt * width), BF16),
        pltpu.VMEM((out_cols, nt * width), BF16),
        pltpu.VMEM((length, nt * width), BF16),
        pltpu.VMEM((length, nt * width), BF16),
        pltpu.VMEM((nt, 8, length), F32),
        pltpu.VMEM((length, features), BF16),
        pltpu.VMEM((length, 5 * width), F32),
        pltpu.VMEM((length, width), BF16),
        pltpu.VMEM((2, edge, width), BF16),
        pltpu.VMEM((length + 2 * edge, width), F32),
        pltpu.VMEM((length, width), F32),
        pltpu.VMEM((length, width), F32),
        pltpu.VMEM((2, length, width), BF16),
        pltpu.VMEM((2, width, 2 * width), BF16),
        pltpu.VMEM((2, SPAN, width, 2 * width), BF16),
        pltpu.VMEM((2, width, 2 * width), F32),
        pltpu.VMEM((2, width, 2 * width), BF16),
        pltpu.VMEM((2, blocks, width, 2 * width), BF16),
        pltpu.VMEM((2, width, width), F32),
        pltpu.VMEM((2, width, width), BF16),
        pltpu.VMEM((2, width, width), BF16),
        dma((7,)),
        dma((2, ups, PARTS)),
        dma((2, ups, PARTS)),
        dma((2, ups)),
        dma((2, ups)),
        dma((2, nt - 1)),
        dma((2, nt - 1)),
        dma((2,)),
        dma((2,)),
        dma((nt - 1,)),
        dma((nt - 1,)),
        dma((nt - 1,)),
        dma((nt - 1,)),
        dma((nt - 1,)),
        dma((nt - 1,)),
        dma((2, SPAN - 1)),
        dma((2, SPAN - 1)),
        dma((2, max(blocks - 2, 1))),
        dma((2, max(blocks - 2, 1))),
        dma((2, SPAN)),
        dma((2,)),
    ]
    return pl.pallas_call(
        functools.partial(layer_kernel, nz, nt),
        name="layer",
        out_shape=jax.ShapeDtypeStruct((length, out_cols), BF16),
        in_specs=[vmem, vmem, hbm, hbm, hbm, vmem, hbm, hbm, vmem, vmem, vmem, vmem, vmem, hbm, hbm],
        out_specs=vmem,
        scratch_shapes=scratch,
        compiler_params=pltpu.CompilerParams(
            collective_id=0, has_side_effects=True, vmem_limit_bytes=48 * 1024 * 1024
        ),
    )(
        tokens_in,
        input_gain.reshape(1, -1),
        w_query,
        w_key,
        w_value,
        w_gates,
        w_glu_value,
        sigmoid_opener_matrix,
        log_decay,
        head_gain.reshape(1, -1),
        conv_kernel,
        norm_gain.reshape(1, -1),
        norm_shift.reshape(1, -1),
        out_delta,
        out_conv,
    )


def solution(mesh):
    placed = (
        P(("grp", "sp"), None),
        P(),
        P("sp", "tp"),
        P("sp", "tp"),
        P("sp", "tp"),
        P("sp", "tp"),
        P("sp", "tp"),
        P("sp", "tp"),
        P(("grp", "sp"), "tp"),
        P(),
        P(None, "tp"),
        P("tp"),
        P("tp"),
        P(None, "tp"),
        P(None, "tp"),
    )
    return jax.shard_map(
        functools.partial(on_device, mesh.shape["sp"], mesh.shape["tp"]),
        mesh=mesh,
        in_specs=placed,
        out_specs=P(("grp", "sp"), "tp"),
        check_vma=False,
    )
```
